32 devices in a mesh: ep: 16 (over z, x, core), tp: 2 (over y).
Axes of the slice: x: 2, y: 2, z: 4, core: 2. Of those that a mesh axis runs over, the one named last changes fastest.
Arguments:
- hidden_in: bfloat16 [256, 2048], P('ep'), may hold values from -6 to 6
- state_in: float32 [256, 16, 64, 64], P('ep', 'tp'), may hold values from -6 to 6
- receptance: bfloat16 [256, 1024], P('ep', 'tp'), may hold values from -6 to 6
- key_in: bfloat16 [256, 1024], P('ep', 'tp'), may hold values from -1.5 to 1.5
- value_in: bfloat16 [256, 1024], P('ep', 'tp'), may hold values from -6 to 6
- learn_in: bfloat16 [256, 1024], P('ep', 'tp'), may hold values from -8 to 8
- decay_in: float32 [256, 1024], P('ep', 'tp'), may hold values from -6 to 6
- decay_base: float32 [1024], P('tp'), may hold values from -3 to 1
- norm_gain: float32 [1024], P('tp'), may hold values from 0.1 to 1.9
- out_weight: bfloat16 [1024, 2048], P('tp'), may hold values from -0.1875 to 0.1875
- routed_gain: float32 [2048], replicated, may hold values from 0.1 to 1.9
- expert_gate: bfloat16 [16, 2048, 512], P('ep', None, 'tp'), may hold values from -0.125 to 0.125
- expert_up: bfloat16 [16, 2048, 512], P('ep', None, 'tp'), may hold values from -0.125 to 0.125
- expert_down: bfloat16 [16, 512, 2048], P('ep', 'tp'), may hold values from -0.25 to 0.25
- route_ids: int32 [256, 6], P('ep'), may hold values from 0 to 15, all different within a row; in each aligned block of 16 rows (0 to 15, 16 to 31, ...) at most 12 rows name the same one
- route_weights: float32 [256, 6], P('ep'), may hold values from 0.05 to 0.5
Outputs:
- hidden_out: bfloat16 [256, 2048], P('ep')
- state_out: float32 [256, 16, 64, 64], P('ep', 'tp')
The draws below stay inside these ranges and needn't reach their ends.
Inputs may be any that keep to these rules, and one draw needn't show every extreme that they name: `route_ids`: each row names 6 different experts. Among the rows of one index of ep no expert is named more than 12 times, a bound that some block reaches.
All inputs are finite; a program needn't handle non-finite values.
Results may differ from the reference program's by a relative error of at most 0.014.
Values may be sent and summed in bfloat16 or wider, within the bound.
A program may use at most 128 MiB of HBM per device.

```python
import math
import jax
import jax.numpy as jnp
import numpy as np
from jax import lax

D = 2048
HEADS = 16
HEAD_DIM = 64
RD = 1024
FF = 512
EXPERTS = 16
TOP_K = 6
SEQ_DEV = 16
SEQS = 256
CAP = 12
N_EP = 16
N_TP = 2


def level_of(own_key, dims, shards, low, largest):
    loudness, own = 1.0, jax.random.fold_in(own_key, 6)
    for dim, shards_of in shards:
        draws = jnp.exp(jax.random.uniform(jax.random.fold_in(own, dim), (shards_of,), jnp.float32, low / len(shards), largest / len(shards)))
        loudness = loudness * jnp.repeat(draws, dims[dim] // shards_of).reshape([-1 if axis == dim else 1 for axis in range(len(dims))])
    return loudness


def assign_block(rng, own, number, rows, number_of, top, most, lean):
    sequence = jax.random.permutation(rng, number_of)
    packed, ordinary = shares(number_of, rows * top, most, lean, True), shares(number_of, rows * top, most, lean, False)
    places = jnp.arange(number_of)

    def named(tallies, rotation):
        used = int((tallies > 0).sum())
        fixed = max(1, used // 4)
        shifted = fixed + (places - fixed + rotation * (used - fixed)) % max(1, number_of - fixed)
        return jnp.zeros((number_of,), jnp.int32).at[sequence[jnp.where(places < fixed, places, shifted)]].set(jnp.asarray(tallies, jnp.int32))

    tallies = jnp.where(number % 4 == 0, named(packed, number // 4), named(ordinary, number - number // 4 - 1))
    mixed = jax.random.permutation(jax.random.fold_in(own, 3), number_of)
    source_of, receiver = mixed[0:number_of // 2 * 2:2], mixed[1:number_of // 2 * 2:2]
    margin = jnp.minimum(tallies[source_of] - 1, most - tallies[receiver]) // 2
    margin = jnp.where((source_of == sequence[0]) | (receiver == sequence[0]) | (tallies[receiver] == 0), 0, jnp.maximum(margin, 0))
    shifted = jax.random.randint(jax.random.fold_in(own, 4), (number_of // 2,), 0, 1 << 20) % (margin + 1)
    tallies = tallies.at[source_of].add(-shifted).at[receiver].add(shifted)
    members = jnp.searchsorted(jnp.cumsum(tallies), jnp.arange(rows * top), side="right").astype(jnp.int32)
    listing = members.reshape(top, rows).T
    listing = listing[jax.random.permutation(jax.random.fold_in(own, 1), rows)]
    rotation = jax.random.randint(jax.random.fold_in(own, 2), (rows, 1), 0, top)
    return jnp.take_along_axis(listing, (jnp.arange(top)[None, :] + rotation) % top, axis=1)


def shares(amount, total, limit, slope, full):
    weights = [(1 << 20) // math.isqrt(grade ** slope) + 1 for grade in range(1, amount + 1)]
    largest = limit if full else min(limit, max(-(-total // amount), total * weights[0] // sum(weights)))
    least = 1 if total - largest >= amount - 1 else 0
    given, rest = [largest] + [least] * (amount - 1), total - largest - least * (amount - 1)
    while rest > 0:
        candidates = [i for i in range(1, amount) if given[i] < largest] or [i for i in range(1, amount) if given[i] < limit]
        mass, remaining = sum([weights[i] for i in candidates]), rest
        for i in candidates:
            extra = min(limit - given[i], max(1, remaining * weights[i] // mass), rest)
            given[i] = given[i] + extra
            rest = rest - extra
    return np.array(given)


def centred(key, dims, deviation, limit, cuts=(), held_as=jnp.bfloat16):
    values = jax.random.normal(key, dims, jnp.float32) * deviation
    if len(cuts) > 0:
        values = level_of(key, dims, cuts, -0.22, 0.18) * values
    return jnp.clip(values, min=-limit, max=limit).astype(held_as)


def setup_inputs(seed: int = 0) -> dict:
    seeds = jax.random.split(jax.random.key(seed), 17)
    hidden_in = centred(seeds[0], (SEQS, D), 1.0, 6.0, ((0, 16),))
    state_in = centred(seeds[1], (SEQS, HEADS, HEAD_DIM, HEAD_DIM), 1.0, 6.0, ((0, 16), (1, 2)), jnp.float32)
    receptance = centred(seeds[2], (SEQS, RD), 1.0, 6.0, ((0, 16), (1, 2)))
    key_in = centred(seeds[3], (SEQS, RD), 0.25, 1.5, ((0, 16), (1, 2)))
    value_in = centred(seeds[4], (SEQS, RD), 1.0, 6.0, ((0, 16), (1, 2)))
    learn_in = centred(seeds[5], (SEQS, RD), 2.0, 8.0, ((0, 16), (1, 2)))
    decay_in = centred(seeds[6], (SEQS, RD), 1.0, 6.0, ((0, 16), (1, 2)), jnp.float32)
    decay_base = jnp.clip(-3.0 + 4.0 * jax.random.uniform(seeds[7], (RD,), jnp.float32) ** level_of(seeds[7], (RD,), ((0, 2),), -0.2, 0.2), -3.0, 1.0)
    norm_gain = jnp.clip(1.0 + 0.18 * jax.random.normal(seeds[8], (RD,), jnp.float32), 0.1, 1.9)
    out_weight = centred(seeds[9], (RD, D), RD ** -0.5, 0.1875, ((0, 2),))
    routed_gain = jnp.clip(1.0 + 0.18 * jax.random.normal(seeds[10], (D,), jnp.float32), 0.1, 1.9)
    expert_gate = centred(seeds[11], (EXPERTS, D, FF), D ** -0.5, 0.125, ((0, 16), (2, 2)))
    expert_up = centred(seeds[12], (EXPERTS, D, FF), D ** -0.5, 0.125, ((0, 16), (2, 2)))
    expert_down = centred(seeds[13], (EXPERTS, FF, D), FF ** -0.5, 0.25, ((0, 16), (1, 2)))
    route_ids_keys = jax.random.split(jax.random.fold_in(seeds[14], 1), SEQS // SEQ_DEV)
    route_ids_turns = jax.random.permutation(jax.random.fold_in(seeds[14], 3), SEQS // SEQ_DEV)
    route_ids = jax.vmap(lambda own, number: assign_block(jax.random.fold_in(seeds[14], 2), own, number, SEQ_DEV, EXPERTS, TOP_K, CAP, 2))(route_ids_keys, route_ids_turns).reshape((SEQS, TOP_K))
    route_weights = jnp.clip(jnp.exp(math.log(0.5) - 2.3025851 * jax.random.uniform(seeds[15], (SEQS, TOP_K), jnp.float32) ** level_of(seeds[15], (SEQS, TOP_K), ((0, 16),), -0.2, 0.2)), 0.05, 0.5)
    return {"hidden_in": hidden_in, "state_in": state_in, "receptance": receptance, "key_in": key_in, "value_in": value_in, "learn_in": learn_in, "decay_in": decay_in, "decay_base": decay_base, "norm_gain": norm_gain, "out_weight": out_weight, "routed_gain": routed_gain, "expert_gate": expert_gate, "expert_up": expert_up, "expert_down": expert_down, "route_ids": route_ids, "route_weights": route_weights}


EPSILON = 1e-06
GROUP_EPSILON = 0.00064

def heads_update(state_in, receptance, key_in, value_in, learn_in, decay_in, decay_base, norm_gain):
    seq_count = receptance.shape[0]
    head_count = state_in.shape[1]
    head_size = state_in.shape[3]

    def to_heads(values):
        return values.astype(jnp.float32).reshape(seq_count, head_count, head_size)
    reading = to_heads(receptance)
    keys = to_heads(key_in)
    values = to_heads(value_in)
    learning = jax.nn.sigmoid(to_heads(learn_in))
    log_rate = -jax.nn.softplus(-(decay_base[None, :] + decay_in)) - 0.5
    decay = to_heads(jnp.exp(-jnp.exp(log_rate)))
    unit_key = keys * lax.rsqrt(lax.optimization_barrier(jnp.sum(keys * keys, axis=-1, keepdims=True)) + EPSILON)
    carried = jnp.einsum('shij,shj->shi', state_in, unit_key, precision=lax.Precision.HIGHEST)
    new_state = state_in * decay[:, :, None, :] - carried[..., None] * (unit_key * learning)[:, :, None, :] + values[..., None] * keys[:, :, None, :]
    output = jnp.einsum('shij,shj->shi', new_state, reading, precision=lax.Precision.HIGHEST)
    center = lax.optimization_barrier(jnp.mean(output, axis=-1, keepdims=True))
    spread = lax.optimization_barrier(jnp.mean(jnp.square(output - center), axis=-1, keepdims=True))
    gain = norm_gain.astype(jnp.float32).reshape(head_count, head_size)
    normed = (output - center) * lax.rsqrt(spread + GROUP_EPSILON) * gain[None]
    return (normed.reshape(seq_count, head_count * head_size).astype(jnp.bfloat16), new_state)

def expert_rows(rows, gate_weight, up_weight, down_weight):
    gate = jnp.dot(rows, gate_weight, preferred_element_type=jnp.float32)
    upward = jnp.dot(rows, up_weight, preferred_element_type=jnp.float32)
    hidden = (jax.nn.silu(gate) * upward).astype(jnp.bfloat16)
    block = hidden.shape[1] // N_TP
    partial_value = jnp.einsum('bjf,jfd->jbd', hidden.reshape(hidden.shape[0], N_TP, block).astype(jnp.float32), down_weight.reshape(N_TP, block, down_weight.shape[1]).astype(jnp.float32))
    rounded = lax.optimization_barrier(partial_value.astype(jnp.bfloat16)).astype(jnp.float32)
    return lax.optimization_barrier(jnp.sum(rounded, axis=0)).astype(jnp.bfloat16)

def reference(hidden_in, state_in, receptance, key_in, value_in, learn_in, decay_in, decay_base, norm_gain, out_weight, routed_gain, expert_gate, expert_up, expert_down, route_ids, route_weights):
    mixed, new_state = heads_update(state_in, receptance, key_in, value_in, learn_in, decay_in, decay_base, norm_gain)
    seq_total = hidden_in.shape[0]
    block = mixed.shape[1] // N_TP
    partial_value = jnp.einsum('sjg,jgd->jsd', mixed.reshape(seq_total, N_TP, block).astype(jnp.float32), out_weight.reshape(N_TP, block, out_weight.shape[1]).astype(jnp.float32))
    rounded = lax.optimization_barrier(partial_value.astype(jnp.bfloat16)).astype(jnp.float32)
    attention = lax.optimization_barrier(jnp.sum(rounded, axis=0)).astype(jnp.bfloat16)
    residual = hidden_in.astype(jnp.float32) + attention.astype(jnp.float32)
    scale = lax.rsqrt(lax.optimization_barrier(jnp.mean(residual * residual, axis=-1, keepdims=True)) + EPSILON)
    normed = (residual * scale * routed_gain[None, :]).astype(jnp.bfloat16)
    flat_ids = route_ids.reshape(-1).astype(jnp.int32)
    expert_count = expert_gate.shape[0]
    order = jnp.argsort(flat_ids, stable=True).astype(jnp.int32)
    counts = lax.optimization_barrier(jnp.sum((flat_ids[:, None] == jnp.arange(expert_count, dtype=jnp.int32)[None, :]).astype(jnp.int32), axis=0))
    starts = (jnp.cumsum(counts) - counts).astype(jnp.int32)
    window = N_EP * CAP
    padded_order = jnp.concatenate([order, jnp.zeros((window,), jnp.int32)])
    flat_weights = route_weights.reshape(-1)

    def visit(total, expert):
        chosen = lax.dynamic_slice_in_dim(padded_order, starts[expert], window, 0)
        tokens = chosen // TOP_K
        live = jnp.arange(window, dtype=jnp.int32) < counts[expert]
        result = expert_rows(normed[tokens], expert_gate[expert], expert_up[expert], expert_down[expert])
        weight = jnp.where(live, flat_weights[chosen], jnp.zeros_like(flat_weights[chosen]))
        return (total.at[tokens].add(weight[:, None] * result.astype(jnp.float32)), None)
    routed, _ = lax.scan(visit, jnp.zeros_like(residual), jnp.arange(expert_count, dtype=jnp.int32))
    return ((residual + routed).astype(jnp.bfloat16), new_state)
```

```python
import functools

import jax
import jax.numpy as jnp
from jax import lax
from jax.experimental import pallas as pl
from jax.experimental.pallas import tpu as pltpu
from jax.sharding import PartitionSpec as P

EPSILON = 1e-06
GROUP_EPSILON = 0.00064
MESH = pl.DeviceIdType.MESH
F32 = jnp.float32
BF16 = jnp.bfloat16
LANES = 128


def split(value):
    high = value.astype(BF16)
    return high, (value - high.astype(F32)).astype(BF16)


def one_head(wide, head, size):
    first = head * size // LANES * LANES
    tile = wide[:, first:first + max(LANES, size)]
    offset = head * size - first
    return (pltpu.roll(tile, tile.shape[1] - offset, 1) if offset else tile)[:, :size]


def head_vectors(read_ref, key_ref, value_ref, learn_ref, decay_ref, base_ref, heads, size):
    reading = read_ref[...].astype(F32)
    keys = key_ref[...].astype(F32)
    values = value_ref[...].astype(F32)
    learning = jax.nn.sigmoid(learn_ref[...].astype(F32))
    decay = jnp.exp(-jax.nn.sigmoid(base_ref[...] + decay_ref[...]) * jnp.exp(F32(-0.5)))
    vectors = []
    for head in range(heads):
        key, read, keep, value, learn = (
            one_head(wide, head, size) for wide in (keys, reading, decay, values, learning)
        )
        unit = key * lax.rsqrt(jnp.sum(key * key, axis=-1, keepdims=True) + EPSILON)
        learned = unit * learn
        learned_read = jnp.sum(learned * read, axis=-1, keepdims=True)
        key_read = jnp.sum(key * read, axis=-1, keepdims=True)
        unit_high, unit_low = split(unit)
        read_high, read_low = split(keep * read)
        probe = jnp.concatenate([unit_high, read_high, unit_low, read_low], axis=0)
        vectors.append((probe, value, learned, keep, key, learned_read, key_read * value))
    return vectors


def own_lanes(seqs, size):
    row = lax.broadcasted_iota(jnp.int32, (seqs, seqs * size), 0)
    lane = lax.broadcasted_iota(jnp.int32, (seqs, seqs * size), 1)
    return row == lane // size


def folded(wide, size):
    step = max(LANES, size)
    total = wide[:, :step]
    for first in range(step, wide.shape[1], step):
        total += wide[:, first:first + step]
    for part in range(1, step // size):
        total += pltpu.roll(total, step // 2, 1) if part == step // size // 2 else 0.0
    return total[:, :size]


def read_head(state, vectors, own):
    seqs, size = vectors[1].shape
    probe = vectors[0]
    high, low = split(state.reshape(seqs * size, size))
    along = (((1,), (1,)), ((), ()))
    first = lax.dot_general(probe, high, along, preferred_element_type=F32)
    second = lax.dot_general(probe[:2 * seqs], low, along, preferred_element_type=F32)
    both = first[:2 * seqs] + first[2 * seqs:] + second
    carried = jnp.where(own, both[:seqs], 0.0)
    kept = jnp.where(own, both[seqs:], 0.0)
    output = folded(kept, size) - folded(carried, size) * vectors[5] + vectors[6]
    return carried, output


def update_head(state, carried, vectors, own):
    _, value, learned, keep, key = vectors[:5]
    seqs, size = value.shape
    carried_high, carried_low = split(carried)
    learned_high, learned_low = split(learned)
    twice = jnp.concatenate([value] * max(1, LANES // size), axis=1)
    spread = jnp.concatenate([twice] * (seqs * size // twice.shape[1]), axis=1)
    spread = jnp.where(own, spread, 0.0).astype(BF16)
    left = jnp.concatenate([carried_high, carried_low, carried_high, spread], axis=0)
    right = jnp.concatenate(
        [-learned_high, -learned_high, -learned_low, key.astype(BF16)], axis=0)
    change = lax.dot_general(left, right, (((0,), (0,)), ((), ())), preferred_element_type=F32)
    return state * keep[:, None, :] + change.reshape(seqs, size, size)


def mix(outputs, gain_ref):
    size = outputs[0].shape[1]
    mixed = []
    for head, output in enumerate(outputs):
        center = jnp.mean(output, axis=-1, keepdims=True)
        spread = jnp.mean(jnp.square(output - center), axis=-1, keepdims=True)
        gain = one_head(gain_ref[...], head, size)
        mixed.append((output - center) * lax.rsqrt(spread + GROUP_EPSILON) * gain)
    return jnp.concatenate(mixed, axis=1).astype(BF16)


def layer_kernel(
    ep, tp, inner,
    state_hbm, read_hbm, key_hbm, value_hbm, learn_hbm, decay_hbm, base_hbm, norm_hbm, weight_hbm,
    hidden_hbm, gain_hbm, ids_hbm, shares_hbm, gate_hbm, up_hbm, down_hbm,
    out_ref, new_ref,
    state_ref, read_ref, key_ref, value_ref, learn_ref, decay_ref, base_ref, norm_ref, weight_ref,
    hidden_ref, gain_ref, ids_ref, shares_ref, carried_ref,
    gate, up, down, heads_in, residual, rows, shares, parts, from_core, summed, from_x, crossed,
    from_z, routed_in,
    vector_sem, state_sem, weight_sem, load_sem,
    heads_send, heads_recv, share_send, share_recv, z_send, x_send, core_send, row_recv,
    core2_send, core2_recv, x2_send, x2_recv, z2_send, z2_recv, routed_send, routed_recv,
):
    width = inner // 2
    outer = ep // inner
    half = ep // 2
    me, member = lax.axis_index("ep"), lax.axis_index("tp")
    z = lax.div(me, inner)
    x = lax.div(lax.rem(me, inner), 2)
    core = lax.rem(me, 2)
    other = 1 - core

    def device(z_at, x_at, core_at):
        return z_at * inner + x_at * 2 + core_at

    def place(z_at, x_at, core_at):
        return core_at * half + z_at * width + x_at

    def send(src, dst, send_sem, recv_sem, ep_at, tp_at=None):
        copy = pltpu.make_async_remote_copy(
            src_ref=src, dst_ref=dst, send_sem=send_sem, recv_sem=recv_sem,
            device_id=(ep_at, member if tp_at is None else tp_at), device_id_type=MESH,
        )
        copy.start()
        return copy

    def arrived(ref, sem):
        pltpu.make_async_remote_copy(
            src_ref=ref, dst_ref=ref, send_sem=sem, recv_sem=sem,
            device_id=(me, member), device_id_type=MESH,
        ).wait_recv()

    vector_pairs = [
        (read_hbm, read_ref), (key_hbm, key_ref), (value_hbm, value_ref), (learn_hbm, learn_ref),
        (decay_hbm, decay_ref), (base_hbm, base_ref), (norm_hbm, norm_ref),
        (hidden_hbm, hidden_ref), (gain_hbm, gain_ref), (ids_hbm, ids_ref),
        (shares_hbm, shares_ref),
    ]
    vector_loads = [pltpu.make_async_copy(source, target, vector_sem.at[i])
                    for i, (source, target) in enumerate(vector_pairs)]
    seqs, heads, size, _ = state_hbm.shape
    state_loads = [pltpu.make_async_copy(state_hbm.at[:, head], state_ref.at[head],
                                         state_sem.at[head]) for head in range(heads)]
    weight_load = pltpu.make_async_copy(weight_hbm, weight_ref, weight_sem.at[0])
    loads = [
        pltpu.make_async_copy(gate_hbm.at[0], gate, load_sem.at[0]),
        pltpu.make_async_copy(up_hbm.at[0], up, load_sem.at[1]),
        pltpu.make_async_copy(down_hbm.at[0], down, load_sem.at[2]),
    ]
    for load in vector_loads + state_loads + [weight_load] + loads:
        load.start()
    barrier = pltpu.get_barrier_semaphore()
    for step in range(1, ep):
        pl.semaphore_signal(barrier, inc=1, device_id=(lax.rem(me + step, ep), member),
                            device_id_type=MESH)
    for step in range(1, tp):
        pl.semaphore_signal(barrier, inc=1, device_id=(me, lax.rem(member + step, tp)),
                            device_id_type=MESH)
    for load in vector_loads:
        load.wait()
    vectors = head_vectors(read_ref, key_ref, value_ref, learn_ref, decay_ref, base_ref, heads,
                           size)
    own = own_lanes(seqs, size)
    outputs = []
    for head in range(heads):
        state_loads[head].wait()
        carried, output = read_head(state_ref[head], vectors[head], own)
        carried_ref[head] = carried
        outputs.append(output)
    mixed = mix(outputs, norm_ref)
    weight_load.wait()
    pl.semaphore_wait(barrier, ep - 1 + tp - 1)
    sent = []
    model = rows.shape[2]
    slices = heads_send.shape[0]
    spans = [pl.ds(p * (model // slices), model // slices) for p in range(slices)]
    for p, span in enumerate(spans):
        product = jnp.dot(mixed, weight_ref[:, span], preferred_element_type=F32)
        heads_in[member, :, span] = product.astype(BF16)
        for step in range(1, tp):
            sent.append(send(heads_in.at[member, :, span], heads_in.at[member, :, span],
                             heads_send.at[p, step - 1], heads_recv.at[p, member], me,
                             lax.rem(member + step, tp)))
    mine = place(z, x, core)
    lanes = shares.shape[2]
    lane = lax.broadcasted_iota(jnp.int32, (seqs, lanes), 1)
    down_rows = lax.broadcasted_iota(jnp.int32, (seqs, seqs), 0)
    diagonal = down_rows == lax.broadcasted_iota(jnp.int32, (seqs, seqs), 1)
    table = jnp.zeros((seqs, lanes), F32)
    for k in range(ids_ref.shape[0]):
        named = jnp.where(diagonal, ids_ref[k:k + 1, :].astype(F32), 0.0)
        share = jnp.where(diagonal, shares_ref[k:k + 1, :], 0.0)
        named = jnp.sum(named, axis=-1, keepdims=True)
        share = jnp.sum(share, axis=-1, keepdims=True)
        table += jnp.where(named == lane.astype(F32), share, 0.0)
    shares[mine] = table
    for step in range(1, ep):
        sent.append(send(shares.at[mine], shares.at[mine], share_send.at[step - 1],
                         share_recv.at[mine], lax.rem(me + step, ep)))
    for head in range(heads):
        new_ref[:, head] = update_head(state_ref[head], carried_ref[head], vectors[head], own)
    for p, span in enumerate(spans):
        for step in range(1, tp):
            source = lax.rem(member + step, tp)
            arrived(heads_in.at[source, :, span], heads_recv.at[p, source])
    attention = heads_in[0].astype(F32)
    for t in range(1, tp):
        attention += heads_in[t].astype(F32)
    value = hidden_ref[...].astype(F32) + attention.astype(BF16).astype(F32)
    residual[...] = value
    scale = lax.rsqrt(jnp.mean(value * value, axis=-1, keepdims=True) + EPSILON)
    rows[mine] = (value * scale * gain_ref[...]).astype(BF16)

    def pass_x(block, base):
        for dx in range(1, width):
            sent.append(send(rows.at[block], rows.at[block], x_send.at[base * (width - 1) + dx - 1],
                             row_recv.at[block], device(z, lax.rem(x + dx, width), core)))

    def pass_core(block, base):
        sent.append(send(rows.at[block], rows.at[block], core_send.at[base], row_recv.at[block],
                         device(z, x, other)))

    for dz in range(1, outer):
        sent.append(send(rows.at[mine], rows.at[mine], z_send.at[dz - 1], row_recv.at[mine],
                         device(lax.rem(z + dz, outer), x, core)))
    pass_x(mine, 0)
    pass_core(mine, 0)
    for dz in range(1, outer):
        block = place(lax.rem(z + outer - dz, outer), x, core)
        arrived(rows.at[block], row_recv.at[block])
        pass_x(block, dz)
        pass_core(block, dz)
    count = outer
    for dz in range(outer):
        for dx in range(1, width):
            block = place(lax.rem(z + outer - dz, outer), lax.rem(x + width - dx, width), core)
            arrived(rows.at[block], row_recv.at[block])
            pass_core(block, count)
            count += 1
    for load in loads:
        load.wait()
    for step in range(1, ep):
        peer = lax.rem(me + step, ep)
        block = place(lax.div(peer, inner), lax.div(lax.rem(peer, inner), 2), lax.rem(peer, 2))
        arrived(shares.at[block], share_recv.at[block])

    take = half
    while take * seqs > 256 and take % 2 == 0:
        take //= 2
    chunk_lane = lax.broadcasted_iota(jnp.int32, (take * seqs, lanes), 1)

    def expert(first):
        block = rows[pl.ds(first, take)].reshape(take * seqs, rows.shape[2])
        gated = jnp.dot(block, gate[...], preferred_element_type=F32)
        upward = jnp.dot(block, up[...], preferred_element_type=F32)
        hidden = (jax.nn.silu(gated) * upward).astype(BF16)
        share = shares[pl.ds(first, take)].reshape(take * seqs, lanes)
        share = jnp.sum(jnp.where(chunk_lane == me, share, 0.0), axis=-1, keepdims=True)
        product = jnp.dot(hidden, down[...], preferred_element_type=F32) * share
        parts[pl.ds(first, take)] = product.astype(BF16).reshape(take, seqs, rows.shape[2])

    def experts_of(core_at):
        @pl.loop(0, half // take)
        def _(i):
            expert(core_at * half + i * take)

    experts_of(core)
    for i in range(half):
        block = other * half + i
        arrived(rows.at[block], row_recv.at[block])
    experts_of(other)

    pieces = core2_recv.shape[0]
    cuts = [pl.ds(p * (model // pieces), model // pieces) for p in range(pieces)]
    x_order = list(range(1, width)) + [0]
    z_order = list(range(1, outer)) + [0]
    for p, cut in enumerate(cuts):
        for dx in x_order:
            for dz in z_order:
                spot = lax.rem(z + dz, outer) * width + lax.rem(x + dx, width)
                sent.append(send(parts.at[other * half + spot, :, cut],
                                 from_core.at[spot, :, cut],
                                 core2_send.at[p, dx * outer + dz], core2_recv.at[p, spot],
                                 device(z, x, other)))
    for p, cut in enumerate(cuts):
        for dx in x_order:
            for dz in z_order:
                z_at = lax.rem(z + dz, outer)
                spot = z_at * width + lax.rem(x + dx, width)
                arrived(from_core.at[spot, :, cut], core2_recv.at[p, spot])
                value = (parts[core * half + spot, :, cut].astype(F32)
                         + from_core[spot, :, cut].astype(F32))
                summed[spot, :, cut] = value.astype(BF16)
                if dx:
                    sent.append(send(summed.at[spot, :, cut], from_x.at[dx - 1, z_at, :, cut],
                                     x2_send.at[p, (dx - 1) * outer + dz],
                                     x2_recv.at[p, dx - 1, z_at],
                                     device(z, lax.rem(x + dx, width), core)))
    for p, cut in enumerate(cuts):
        for dz in z_order:
            z_at = lax.rem(z + dz, outer)
            value = summed[z_at * width + x, :, cut].astype(F32)
            for dx in range(1, width):
                arrived(from_x.at[dx - 1, z_at, :, cut], x2_recv.at[p, dx - 1, z_at])
                value += from_x[dx - 1, z_at, :, cut].astype(F32)
            crossed[dz, :, cut] = value.astype(BF16)
            if dz:
                sent.append(send(crossed.at[dz, :, cut], from_z.at[dz - 1, :, cut],
                                 z2_send.at[p, dz - 1], z2_recv.at[p, dz - 1],
                                 device(z_at, x, core)))
    for p, cut in enumerate(cuts):
        value = crossed[0, :, cut].astype(F32)
        for dz in range(1, outer):
            arrived(from_z.at[dz - 1, :, cut], z2_recv.at[p, dz - 1])
            value += from_z[dz - 1, :, cut].astype(F32)
        routed_in[member, :, cut] = value.astype(BF16)
        for step in range(1, tp):
            sent.append(send(routed_in.at[member, :, cut], routed_in.at[member, :, cut],
                             routed_send.at[p, step - 1], routed_recv.at[p, member], me,
                             lax.rem(member + step, tp)))
    for p, cut in enumerate(cuts):
        for step in range(1, tp):
            source = lax.rem(member + step, tp)
            arrived(routed_in.at[source, :, cut], routed_recv.at[p, source])
        routed = routed_in[0, :, cut].astype(F32)
        for t in range(1, tp):
            routed += routed_in[t, :, cut].astype(F32)
        out_ref[:, cut] = (residual[:, cut] + routed).astype(BF16)
    for copy in sent:
        copy.wait_send()


def layer_call(
    inner, state_in, receptance, key_in, value_in, learn_in, decay_in, base, norm, out_weight,
    hidden_in, gain, ids, route_weights, gate, up, down,
):
    ep, tp = lax.axis_size("ep"), lax.axis_size("tp")
    seqs, model = hidden_in.shape
    heads, size = state_in.shape[1:3]
    width, outer, half = inner // 2, ep // inner, ep // 2
    lanes = -(-ep // LANES) * LANES
    hbm = pl.BlockSpec(memory_space=pltpu.HBM)
    block = (seqs, model)
    pieces = 2 if model % (2 * LANES) == 0 else 1
    slices = 4 if model % (4 * LANES) == 0 else 1
    dma = lambda *shape: pltpu.SemaphoreType.DMA(tuple(max(1, n) for n in shape))
    buffer = lambda *lead: pltpu.VMEM(tuple(max(1, n) for n in lead) + block, BF16)
    small = [receptance, key_in, value_in, learn_in, decay_in, base[None], norm[None], out_weight,
             hidden_in, gain[None], ids.T, route_weights.T]
    return pl.pallas_call(
        functools.partial(layer_kernel, ep, tp, inner),
        in_specs=[hbm] * 16,
        out_shape=[pltpu.VMEM(block, BF16), pltpu.VMEM(state_in.shape, F32)],
        scratch_shapes=[
            pltpu.VMEM((heads, seqs, size, size), F32),
            *[pltpu.VMEM(array.shape, array.dtype) for array in small],
            pltpu.VMEM((heads, seqs, seqs * size), F32),
            pltpu.VMEM(gate.shape[1:], BF16),
            pltpu.VMEM(up.shape[1:], BF16),
            pltpu.VMEM(down.shape[1:], BF16),
            buffer(tp),
            pltpu.VMEM(block, F32),
            buffer(ep),
            pltpu.VMEM((ep, seqs, lanes), F32),
            buffer(ep),
            buffer(half),
            buffer(half),
            buffer(width - 1, outer),
            buffer(outer),
            buffer(outer - 1),
            buffer(tp),
            dma(len(small) - 1), dma(heads), dma(1), dma(3),
            dma(slices, tp - 1), dma(slices, tp),
            dma(ep - 1), dma(ep),
            dma(outer - 1), dma(outer * (width - 1)), dma(half), dma(ep),
            dma(pieces, half), dma(pieces, half),
            dma(pieces, (width - 1) * outer), dma(pieces, width - 1, outer),
            dma(pieces, outer - 1), dma(pieces, outer - 1),
            dma(pieces, tp - 1), dma(pieces, tp),
        ],
        compiler_params=pltpu.CompilerParams(
            collective_id=0, has_side_effects=True, vmem_limit_bytes=58 * 1024 * 1024
        ),
    )(state_in, *small, gate, up, down)


def on_device(
    inner, hidden_in, state_in, receptance, key_in, value_in, learn_in, decay_in, decay_base,
    norm_gain, out_weight, routed_gain, expert_gate, expert_up, expert_down, route_ids,
    route_weights,
):
    hidden_out, new_state = layer_call(
        inner, state_in, receptance, key_in, value_in, learn_in, decay_in, decay_base, norm_gain,
        out_weight, hidden_in, routed_gain, route_ids, route_weights, expert_gate, expert_up,
        expert_down,
    )
    return (hidden_out, new_state)


def plane_size(mesh):
    line = mesh.devices.reshape(mesh.shape["ep"], mesh.shape["tp"])[:, 0]
    first = getattr(line[0], "coords", None)
    if first is None:
        return min(4, len(line))
    return sum(1 for d in line if d.coords[2] == first[2])


def solution(mesh):
    in_specs = (
        P("ep", None),
        P("ep", "tp", None, None),
        P("ep", "tp"),
        P("ep", "tp"),
        P("ep", "tp"),
        P("ep", "tp"),
        P("ep", "tp"),
        P("tp"),
        P("tp"),
        P("tp", None),
        P(),
        P("ep", None, "tp"),
        P("ep", None, "tp"),
        P("ep", "tp", None),
        P("ep", None),
        P("ep", None),
    )
    out_specs = (P("ep", None), P("ep", "tp", None, None))
    return jax.shard_map(
        functools.partial(on_device, plane_size(mesh)), mesh=mesh, in_specs=in_specs,
        out_specs=out_specs, check_vma=False,
    )
```
